32 devices in a mesh: sp: 8 (over z, y), tp: 4 (over x, core).
Axes of the slice: x: 2, y: 2, z: 4, core: 2. Of those that a mesh axis runs over, the one named last changes fastest.
Arguments:
- tokens: bfloat16 [4096, 2048], P('sp', 'tp'), may hold values from -400 to 400
- norm_gain: float32 [2048], replicated, may hold values from 0.1 to 1.9
- query_weight: bfloat16 [2048, 1024], P(None, 'tp'), may hold values from -0.37306796 to 0.37306796
- key_weight: bfloat16 [2048, 1024], P(None, 'tp'), may hold values from -0.2625825 to 0.2625825
- value_weight: bfloat16 [2048, 1024], P(None, 'tp'), may hold values from -0.125 to 0.125
- outer_gate_weight: bfloat16 [2048, 1024], P(None, 'tp'), may hold values from -0.125 to 0.125
- inner_gate_weight: bfloat16 [2048, 1024], P(None, 'tp'), may hold values from -0.125 to 0.125
- conv_input_weight: bfloat16 [2048, 1024], P(None, 'tp'), may hold values from -0.125 to 0.125
- conv_taps: float32 [3, 1024], P(None, 'tp'), may hold values from -3.5 to 3.5
- lambdas: float32 [8], P('tp'), may hold values from 0.3 to 0.8
- head_gain: float32 [128], replicated, may hold values from 0.1 to 1.9
- attn_out_weight: bfloat16 [1024, 2048], P(None, 'tp'), may hold values from -0.125 to 0.125
- conv_out_weight: bfloat16 [1024, 2048], P(None, 'tp'), may hold values from -0.125 to 0.125
Outputs:
- mixed_out: bfloat16 [4096, 2048], P('sp', 'tp')
- log_totals: float32 [8, 2, 4096], P('tp', None, 'sp')
The draws below stay inside these ranges and needn't reach their ends.
All inputs are finite; a program needn't handle non-finite values.
Results may differ from the reference program's by a relative error of at most 0.014.
The reference program's roundings to bfloat16 on the way count: a program that leaves them out, or rounds other values in their place, can miss the bound.
Values may be sent and summed in bfloat16 or wider, within the bound.
No kernel may reach another device: no remote copies, remote signals or barrier semaphores. Data moves between devices by JAX's collectives and lax.ppermute only.
A program may use at most 128 MiB of HBM per device.

```python
import jax
import jax.numpy as jnp
from jax import lax

WIDTH = 2048
HEADS = 8
HEAD_DIM = 64
TAPS = 3
TOK_DEV = 512
CHANNELS = 1024
TOKENS = 4096


def drawn_weight(key, salt, fan_in):
    base = jax.random.normal(jax.random.fold_in(key, salt), (WIDTH, CHANNELS), jnp.float32)
    base = jnp.clip(base, -6.0, 6.0) * fan_in ** (-0.5)
    return base.astype(jnp.bfloat16)


def draw_query_weight(key, part):
    return drawn_weight(key, 11, WIDTH / 3.0)


def draw_key_weight(key, part):
    return drawn_weight(key, 12, WIDTH * 1.0)


def draw_tokens(key, part):
    values = jnp.clip(jax.random.normal(jax.random.fold_in(key, 2), (TOKENS, WIDTH), jnp.float32), -6.0, 6.0)
    return values.astype(jnp.bfloat16)


def level_of(stream_key, shape, split, low, largest):
    def one(position, parts):
        heights = jax.random.uniform(jax.random.fold_in(jax.random.fold_in(stream_key, 6), position), (parts,), jnp.float32, low / len(split), largest / len(split))
        return jnp.repeat(jnp.exp(heights), shape[position] // parts).reshape((-1,) + (1,) * (len(shape) - position - 1))

    level = one(*split[0])
    for cut in split[1:]:
        level = level * one(*cut)
    return level


def centred(key, dims, spread, most, split=(), held_as=jnp.bfloat16):
    array = jax.random.normal(key, dims, jnp.float32) * spread
    if len(split) > 0:
        array = level_of(key, dims, split, -0.22, 0.18) * array
    return jnp.clip(array, min=-most, max=most).astype(held_as)


def setup_inputs(seed: int = 0) -> dict:
    streams_of = jax.random.split(jax.random.key(seed), 14)
    return {
        "tokens": draw_tokens(jax.random.fold_in(streams_of[13], 71), 0),
        "norm_gain": jnp.clip(1.0 + 0.18 * jax.random.normal(streams_of[1], (WIDTH,), jnp.float32), 0.1, 1.9),
        "query_weight": draw_query_weight(jax.random.fold_in(streams_of[13], 71), 0),
        "key_weight": draw_key_weight(jax.random.fold_in(streams_of[13], 71), 0),
        "value_weight": centred(streams_of[4], (WIDTH, CHANNELS), WIDTH ** -0.5, 0.125, ((1, 4),)),
        "outer_gate_weight": centred(streams_of[5], (WIDTH, CHANNELS), WIDTH ** -0.5, 0.125, ((1, 4),)),
        "inner_gate_weight": centred(streams_of[6], (WIDTH, CHANNELS), WIDTH ** -0.5, 0.125, ((1, 4),)),
        "conv_input_weight": centred(streams_of[7], (WIDTH, CHANNELS), WIDTH ** -0.5, 0.125, ((1, 4),)),
        "conv_taps": centred(streams_of[8], (TAPS, CHANNELS), TAPS ** -0.5, 3.5, ((1, 4),), jnp.float32),
        "lambdas": jnp.clip(0.3 + 0.5 * jax.random.uniform(streams_of[9], (HEADS,), jnp.float32) ** level_of(streams_of[9], (HEADS,), ((0, 4),), -0.2, 0.2), 0.3, 0.8),
        "head_gain": jnp.clip(1.0 + 0.18 * jax.random.normal(streams_of[10], (2 * HEAD_DIM,), jnp.float32), 0.1, 1.9),
        "attn_out_weight": centred(streams_of[11], (CHANNELS, WIDTH), (2 * CHANNELS) ** -0.5, 0.125, ((1, 4),)),
        "conv_out_weight": centred(streams_of[12], (CHANNELS, WIDTH), (2 * CHANNELS) ** -0.5, 0.125, ((1, 4),)),
    }


NORM_EPS = 1e-06
HEAD_EPS = 1e-05
ROPE_BASE = 500000.0
MASKED = -1e+30
HEAD_SCALE = 0.8

def rotate(field_in, positions):
    half_dim = field_in.shape[-1] // 2
    frequency = ROPE_BASE ** (-jnp.arange(half_dim, dtype=jnp.float32) * 2.0 / field_in.shape[-1])
    angles = positions[:, None] * frequency[None, :]
    cosine = jnp.cos(angles)[:, None, None, :]
    sine_part = jnp.sin(angles)[:, None, None, :]
    first_half = field_in[..., :half_dim]
    second_half = field_in[..., half_dim:]
    return jnp.concatenate([first_half * cosine - second_half * sine_part, second_half * cosine + first_half * sine_part], axis=-1)

def reference(tokens, norm_gain, query_weight, key_weight, value_weight, outer_gate_weight, inner_gate_weight, conv_input_weight, conv_taps, lambdas, head_gain, attn_out_weight, conv_out_weight):
    floats = tokens.astype(jnp.float32)
    inverse_rms = lax.rsqrt(lax.optimization_barrier(jnp.mean(floats * floats, axis=1, keepdims=True)) + NORM_EPS)
    scaled = (floats * norm_gain[None, :]).astype(jnp.bfloat16)

    def project(weight):
        return inverse_rms * jnp.dot(scaled, weight, preferred_element_type=jnp.float32)
    positions = jnp.arange(TOKENS, dtype=jnp.float32)
    queries = rotate(project(query_weight).reshape(TOKENS, HEADS, 2, HEAD_DIM), positions).astype(jnp.bfloat16)
    key_rows = rotate(project(key_weight).reshape(TOKENS, HEADS, 2, HEAD_DIM), positions).astype(jnp.bfloat16)
    values = project(value_weight).astype(jnp.bfloat16).reshape(TOKENS, HEADS, 2 * HEAD_DIM)
    outer_gate = project(outer_gate_weight).astype(jnp.bfloat16)
    inner_gate = project(inner_gate_weight).astype(jnp.bfloat16)
    signal = project(conv_input_weight).astype(jnp.bfloat16)
    conv_in = (inner_gate.astype(jnp.float32) * signal.astype(jnp.float32)).astype(jnp.bfloat16)
    padded = jnp.concatenate([jnp.zeros((TAPS - 1, CHANNELS), jnp.bfloat16), conv_in], axis=0)
    summed = jnp.zeros((TOKENS, CHANNELS), jnp.float32)
    for tap_index in range(TAPS):
        summed = summed + conv_taps[tap_index][None, :] * padded[tap_index:tap_index + TOKENS].astype(jnp.float32)
    conv_out = (outer_gate.astype(jnp.float32) * summed).astype(jnp.bfloat16)
    blocks = TOKENS // TOK_DEV

    def one_block(flat_index):
        head_index = flat_index // blocks
        row_start = (flat_index % blocks * TOK_DEV).astype(jnp.int32)
        query_rows = lax.dynamic_slice_in_dim(queries, row_start, TOK_DEV, 0)
        query_rows = lax.dynamic_index_in_dim(query_rows, head_index, 1, keepdims=False)
        head_keys = lax.dynamic_index_in_dim(key_rows, head_index, 1, keepdims=False)
        head_values = lax.dynamic_index_in_dim(values, head_index, 1, keepdims=False)
        scores = jnp.einsum('qcd,kcd->cqk', query_rows.astype(jnp.float32), head_keys.astype(jnp.float32)) * HEAD_DIM ** (-0.5)
        visible = (row_start + jnp.arange(TOK_DEV, dtype=jnp.int32))[:, None] >= jnp.arange(TOKENS, dtype=jnp.int32)[None, :]
        scores = jnp.where(visible[None], scores, MASKED)
        row_max = lax.optimization_barrier(jnp.max(scores, axis=-1, keepdims=True))
        exponent = jnp.where(visible[None], jnp.exp(scores - row_max), 0.0)
        row_sum = lax.optimization_barrier(jnp.sum(exponent, axis=-1, keepdims=True))
        normalized = exponent / row_sum
        lambda_value = lambdas[head_index]
        weights = (normalized[0] - lambda_value * normalized[1]).astype(jnp.bfloat16)
        head_mix = jnp.dot(weights, head_values, preferred_element_type=jnp.float32)
        normed = head_mix * lax.rsqrt(lax.optimization_barrier(jnp.mean(head_mix * head_mix, axis=-1, keepdims=True)) + HEAD_EPS) * head_gain[None, :] * HEAD_SCALE
        return (normed.astype(jnp.bfloat16), (row_max + jnp.log(row_sum))[..., 0])
    head_rows, log_rows = lax.map(one_block, jnp.arange(HEADS * blocks, dtype=jnp.int32))
    attn_out = jnp.transpose(head_rows.reshape(HEADS, blocks, TOK_DEV, 2 * HEAD_DIM), (1, 2, 0, 3)).reshape(TOKENS, CHANNELS)
    log_totals = jnp.transpose(log_rows.reshape(HEADS, blocks, 2, TOK_DEV), (0, 2, 1, 3)).reshape(HEADS, 2, TOKENS)
    mixed_out = jnp.dot(attn_out, attn_out_weight, preferred_element_type=jnp.float32) + jnp.dot(conv_out, conv_out_weight, preferred_element_type=jnp.float32)
    return (mixed_out.astype(jnp.bfloat16), log_totals)
```

```python
import functools
import math

import jax
import jax.numpy as jnp
from jax import lax
from jax.experimental import pallas as pl
from jax.experimental.pallas import tpu as pltpu
from jax.sharding import PartitionSpec as P

NORM_EPS = 1e-06
HEAD_EPS = 1e-05
ROPE_BASE = 500000.0
MASKED = -1e30
HEAD_SCALE = 0.8
VMEM_BYTES = 56 * 1024 * 1024


def shifted(block, axis, distance):
    devices = range(lax.axis_size(axis))
    route = [(i - distance, i) for i in devices if i - distance in devices]
    return lax.ppermute(block, axis, route)


def turn_tables(positions, head_dim, columns):
    half_dim = head_dim // 2
    frequency = ROPE_BASE ** (-jnp.arange(half_dim, dtype=jnp.float32) * 2.0 / head_dim)
    angles = positions[:, None] * jnp.tile(frequency, columns // half_dim)[None, :]
    sign = jnp.where((jnp.arange(columns) % head_dim) < half_dim, -1.0, 1.0)
    return jnp.cos(angles), jnp.sin(angles) * sign[None, :]


def project_kernel(
    tok_ref, gain_ref, cos_ref, sin_ref, wq, wk, wv, wo, wi, ws,
    q_ref, kv_ref, cin_ref, gate_ref, *, head_dim,
):
    floats = tok_ref[...].astype(jnp.float32)
    squares = jnp.sum(floats * floats, axis=1, keepdims=True)
    inverse_rms = lax.rsqrt(squares / floats.shape[1] + NORM_EPS)
    scaled = (floats * gain_ref[...]).astype(jnp.bfloat16)
    columns = wq.shape[1]
    lanes = cos_ref.shape[1]
    half = head_dim // 2

    def project(w):
        return jnp.dot(scaled, w[...], preferred_element_type=jnp.float32) * inverse_rms

    low = lax.broadcasted_iota(jnp.int32, (floats.shape[0], lanes), 1) % head_dim < half
    cosine = cos_ref[...]
    sine = sin_ref[...]

    def turned(raw):
        parts = []
        for start in range(0, columns, lanes):
            part = raw[:, start : start + lanes]
            other = jnp.where(
                low, pltpu.roll(part, lanes - half, 1), pltpu.roll(part, half, 1)
            )
            parts.append((part * cosine + other * sine).astype(jnp.bfloat16))
        return parts

    for index, part in enumerate(turned(project(wk))):
        kv_ref[:, index * lanes : (index + 1) * lanes] = part
    kv_ref[:, columns:] = project(wv).astype(jnp.bfloat16)
    for index, part in enumerate(turned(project(wq))):
        q_ref[:, index * lanes : (index + 1) * lanes] = part
    inner = project(wi).astype(jnp.bfloat16).astype(jnp.float32)
    signal = project(ws).astype(jnp.bfloat16).astype(jnp.float32)
    cin_ref[...] = (inner * signal).astype(jnp.bfloat16)
    gate_ref[...] = project(wo).astype(jnp.bfloat16)


def project_all(tokens, gain, cosine, sine, weights, head_dim):
    rows, width = tokens.shape
    columns = weights[0].shape[1]
    lanes = cosine.shape[1]
    tile = math.gcd(rows, 256)
    row_block = lambda n: pl.BlockSpec((tile, n), lambda i: (i, 0))
    whole = pl.BlockSpec((width, columns), lambda i: (0, 0))
    shape = lambda n: jax.ShapeDtypeStruct((rows, n), jnp.bfloat16)
    return pl.pallas_call(
        functools.partial(project_kernel, head_dim=head_dim),
        grid=(rows // tile,),
        in_specs=[row_block(width), pl.BlockSpec((1, width), lambda i: (0, 0)),
                  row_block(lanes), row_block(lanes)] + [whole] * 6,
        out_specs=[row_block(columns), row_block(2 * columns), row_block(columns), row_block(columns)],
        out_shape=[shape(columns), shape(2 * columns), shape(columns), shape(columns)],
        compiler_params=pltpu.CompilerParams(
            dimension_semantics=("arbitrary",), vmem_limit_bytes=VMEM_BYTES),
        cost_estimate=pl.CostEstimate(
            flops=12 * rows * width * columns, transcendentals=rows,
            bytes_accessed=2 * (rows * width + 6 * width * columns + 5 * rows * columns)),
        name="project",
    )(tokens, gain, cosine, sine, *weights)


def attend_kernel(
    place_ref, lambda_ref, q_ref, k_ref, v_ref, gain_ref, out_ref, totals_ref, s_ref,
    *, local_rows, block, head_dim,
):
    tile = q_ref.shape[0]
    value_dim = v_ref.shape[1]
    head = pl.program_id(0)
    row_start = place_ref[0] * local_rows + pl.program_id(1) * tile
    full_blocks = row_start // block
    queries = q_ref[...] * jnp.asarray(head_dim ** (-0.5), jnp.bfloat16)
    first = lax.broadcasted_iota(jnp.int32, queries.shape, 1) < head_dim
    zero = jnp.zeros_like(queries)
    stacked = jnp.concatenate(
        [jnp.where(first, queries, zero), jnp.where(first, zero, queries)], axis=0
    )
    groups = range(0, block, 128)

    def scores_of(index):
        keys = k_ref[pl.ds(index * block, block), :]
        return lax.dot_general(
            stacked, keys, (((1,), (1,)), ((), ())), preferred_element_type=jnp.float32
        )

    def lane_max(running, scores):
        for g in groups:
            running = jnp.maximum(running, scores[:, g : g + 128])
        return running

    def score_step(index, running):
        scores = scores_of(index)
        s_ref[:, pl.ds(index * block, block)] = scores
        return lane_max(running, scores)

    running = lax.fori_loop(
        0, full_blocks, score_step, jnp.full((2 * tile, 128), MASKED, jnp.float32)
    )
    scores = scores_of(full_blocks)
    row_ids = lax.broadcasted_iota(jnp.int32, scores.shape, 0) % tile + row_start
    col_ids = lax.broadcasted_iota(jnp.int32, scores.shape, 1) + full_blocks * block
    scores = jnp.where(row_ids >= col_ids, scores, MASKED)
    s_ref[:, pl.ds(full_blocks * block, block)] = scores
    row_max = jnp.max(lane_max(running, scores), axis=1, keepdims=True)

    def exp_step(index, running):
        exponent = jnp.exp(s_ref[:, pl.ds(index * block, block)] - row_max)
        s_ref[:, pl.ds(index * block, block)] = exponent
        for g in groups:
            running = running + exponent[:, g : g + 128]
        return running

    running = lax.fori_loop(
        0, full_blocks + 1, exp_step, jnp.zeros((2 * tile, 128), jnp.float32)
    )
    row_sum = jnp.sum(running, axis=1, keepdims=True)
    totals_ref[0] = row_max + jnp.log(row_sum)
    factor = 1.0 / row_sum
    plus = factor[:tile]
    minus = factor[tile:] * lambda_ref[head]

    def value_step(index, running):
        window = pl.ds(index * block, block)
        weights = s_ref[:tile, window] * plus - s_ref[tile:, window] * minus
        return running + jnp.dot(
            weights.astype(jnp.bfloat16), v_ref[window, :], preferred_element_type=jnp.float32
        )

    head_mix = lax.fori_loop(
        0, full_blocks + 1, value_step, jnp.zeros((tile, value_dim), jnp.float32)
    )
    mean_square = jnp.mean(head_mix * head_mix, axis=1, keepdims=True)
    normed = head_mix * lax.rsqrt(mean_square + HEAD_EPS) * gain_ref[...] * HEAD_SCALE
    out_ref[...] = normed.astype(jnp.bfloat16)


def attend(place, lambdas, queries, keys_values, head_gain, head_dim):
    local_rows, columns = queries.shape
    tokens_all = keys_values.shape[0]
    heads = lambdas.shape[0]
    value_dim = 2 * head_dim
    tile = math.gcd(local_rows, 256)
    if tokens_all * tile * 8 > 16 * 1024 * 1024:
        tile = math.gcd(local_rows, 128)
    block = math.gcd(local_rows, 512)
    block = max(block, tile)
    tiles = local_rows // tile
    smem = pl.BlockSpec(memory_space=pltpu.SMEM)
    out, totals = pl.pallas_call(
        functools.partial(attend_kernel, local_rows=local_rows, block=block, head_dim=head_dim),
        grid=(heads, tiles),
        in_specs=[
            smem, smem,
            pl.BlockSpec((tile, value_dim), lambda h, i: (i, h)),
            pl.BlockSpec((tokens_all, value_dim), lambda h, i: (0, h)),
            pl.BlockSpec((tokens_all, value_dim), lambda h, i: (0, heads + h)),
            pl.BlockSpec((1, value_dim), lambda h, i: (0, 0)),
        ],
        out_specs=[
            pl.BlockSpec((tile, value_dim), lambda h, i: (i, h)),
            pl.BlockSpec((1, 2 * tile, 1), lambda h, i: (h * tiles + i, 0, 0)),
        ],
        out_shape=[
            jax.ShapeDtypeStruct((local_rows, columns), jnp.bfloat16),
            jax.ShapeDtypeStruct((heads * tiles, 2 * tile, 1), jnp.float32),
        ],
        scratch_shapes=[pltpu.VMEM((2 * tile, tokens_all), jnp.float32)],
        compiler_params=pltpu.CompilerParams(
            dimension_semantics=("arbitrary", "arbitrary"), vmem_limit_bytes=VMEM_BYTES),
        cost_estimate=pl.CostEstimate(
            flops=8 * heads * local_rows * tokens_all * value_dim,
            transcendentals=2 * heads * local_rows * tokens_all,
            bytes_accessed=4 * tokens_all * columns),
        name="attend",
    )(place, lambdas, queries, keys_values, keys_values, head_gain)
    totals = totals.reshape(heads, tiles, 2, tile).transpose(0, 2, 1, 3)
    return out, totals.reshape(heads, 2, local_rows)


def per_device(
    tokens,
    norm_gain,
    query_weight,
    key_weight,
    value_weight,
    outer_gate_weight,
    inner_gate_weight,
    conv_input_weight,
    conv_taps,
    lambdas,
    head_gain,
    attn_out_weight,
    conv_out_weight,
):
    local_rows = tokens.shape[0]
    local_heads = lambdas.shape[0]
    head_dim = query_weight.shape[1] // (2 * local_heads)
    taps_count = conv_taps.shape[0]
    columns_dev = query_weight.shape[1]
    place = lax.axis_index("sp").astype(jnp.int32)
    positions = (
        place * local_rows + jnp.arange(local_rows, dtype=jnp.int32)
    ).astype(jnp.float32)
    cosine, sine = turn_tables(positions, head_dim, 2 * head_dim)
    queries, keys_values, conv_in, outer_gate = project_all(
        lax.all_gather(tokens, "tp", axis=1, tiled=True),
        norm_gain[None, :], cosine, sine,
        (query_weight, key_weight, value_weight, outer_gate_weight,
         inner_gate_weight, conv_input_weight),
        head_dim,
    )
    all_keys_values = lax.all_gather(keys_values, "sp", axis=0, tiled=True)
    rim_rows = shifted(conv_in[local_rows - (taps_count - 1) :], "sp", 1)
    padded = jnp.concatenate([rim_rows, conv_in], axis=0)
    summed = jnp.zeros((local_rows, columns_dev), jnp.float32)
    for tap_index in range(taps_count):
        summed = summed + conv_taps[tap_index][None, :] * padded[
            tap_index : tap_index + local_rows
        ].astype(jnp.float32)
    conv_out = (outer_gate.astype(jnp.float32) * summed).astype(jnp.bfloat16)
    conv_all = lax.all_gather(conv_out, "tp", axis=1, tiled=True)
    attn_out, log_totals = attend(
        place[None], lambdas, queries, all_keys_values, head_gain[None, :], head_dim
    )
    conv_part = jnp.dot(conv_all, conv_out_weight, preferred_element_type=jnp.float32)
    mixed_out = conv_part + jnp.dot(
        lax.all_gather(attn_out, "tp", axis=1, tiled=True),
        attn_out_weight,
        preferred_element_type=jnp.float32,
    )
    return (mixed_out.astype(jnp.bfloat16), log_totals)


def solution(mesh):
    in_specs = (
        P("sp", "tp"),
        P(),
        P(None, "tp"),
        P(None, "tp"),
        P(None, "tp"),
        P(None, "tp"),
        P(None, "tp"),
        P(None, "tp"),
        P(None, "tp"),
        P("tp"),
        P(),
        P(None, "tp"),
        P(None, "tp"),
    )
    out_specs = (P("sp", "tp"), P("tp", None, "sp"))
    return jax.shard_map(
        per_device, mesh=mesh, in_specs=in_specs, out_specs=out_specs, check_vma=False
    )
```

```python
import functools
import math

import jax
import jax.numpy as jnp
from jax import lax
from jax.experimental import pallas as pl
from jax.experimental.pallas import tpu as pltpu
from jax.sharding import PartitionSpec as P

NORM_EPS = 1e-06
HEAD_EPS = 1e-05
ROPE_BASE = 500000.0
MASKED = -1e30
HEAD_SCALE = 0.8
VMEM_BYTES = 56 * 1024 * 1024


def shifted(block, axis, distance):
    devices = range(lax.axis_size(axis))
    route = [(i - distance, i) for i in devices if i - distance in devices]
    return lax.ppermute(block, axis, route)


def turn_tables(positions, head_dim, columns):
    half_dim = head_dim // 2
    frequency = ROPE_BASE ** (-jnp.arange(half_dim, dtype=jnp.float32) * 2.0 / head_dim)
    angles = positions[:, None] * jnp.tile(frequency, columns // half_dim)[None, :]
    sign = jnp.where((jnp.arange(columns) % head_dim) < half_dim, -1.0, 1.0)
    return jnp.cos(angles), jnp.sin(angles) * sign[None, :]


def tp_pieces(block):
    size = lax.axis_size("tp")
    here = lax.axis_index("tp").astype(jnp.int32)
    if size == 4:
        far = lax.ppermute(block, "tp", [(i, i ^ 2) for i in range(4)])
        near = lax.ppermute(block, "tp", [(i, i ^ 1) for i in range(4)])
        both = lax.ppermute(far, "tp", [(i, i ^ 1) for i in range(4)])
        return [block, near, far, both], [here, here ^ 1, here ^ 2, here ^ 3]
    gathered = lax.all_gather(block, "tp", axis=0, tiled=False)
    return [gathered[i] for i in range(size)], [jnp.int32(i) for i in range(size)]


def project_kernel(*refs, head_dim, pieces, heads):
    source_ref, member_ref = refs[:2]
    tokens = refs[2 : 2 + pieces]
    gain_ref, cos_ref, sin_ref, wq, wk, wv, wo, wi, ws = refs[2 + pieces : 11 + pieces]
    outs = refs[11 + pieces :]
    q_refs, kv_refs = outs[:heads], outs[heads : 2 * heads]
    cin_ref, gate_ref = outs[2 * heads :]
    part_width = tokens[0].shape[1]
    width = part_width * pieces
    rows = tokens[0].shape[0]
    squares = jnp.zeros((rows, 1), jnp.float32)
    scaled = []
    windows = []
    for index in range(pieces):
        start = pl.multiple_of(source_ref[index] * part_width, part_width)
        floats = tokens[index][...].astype(jnp.float32)
        squares = squares + jnp.sum(floats * floats, axis=1, keepdims=True)
        gain = gain_ref[source_ref[index]]
        scaled.append((floats * gain).astype(jnp.bfloat16))
        windows.append(pl.ds(start, part_width))
    inverse_rms = lax.rsqrt(squares / width + NORM_EPS)
    lanes = 2 * head_dim
    half = head_dim // 2

    def project(w):
        total = jnp.dot(scaled[0], w[windows[0], :], preferred_element_type=jnp.float32)
        for index in range(1, pieces):
            total = total + jnp.dot(
                scaled[index], w[windows[index], :], preferred_element_type=jnp.float32
            )
        return total * inverse_rms

    low = lax.broadcasted_iota(jnp.int32, (rows, lanes), 1) % head_dim < half
    cosine = cos_ref[...]
    sine = sin_ref[...]

    def turned(part):
        other = jnp.where(low, pltpu.roll(part, lanes - half, 1), pltpu.roll(part, half, 1))
        return (part * cosine + other * sine).astype(jnp.bfloat16)

    keys = project(wk)
    values = project(wv).astype(jnp.bfloat16)
    queries = project(wq)
    for head in range(heads):
        columns = slice(head * lanes, (head + 1) * lanes)
        key_part = turned(keys[:, columns])
        query_part = turned(queries[:, columns])
        value_part = values[:, columns]
        for slot in range(heads):

            @pl.when((member_ref[0] + slot) % heads == head)
            def _():
                kv_refs[slot][:, :lanes] = key_part
                kv_refs[slot][:, lanes:] = value_part
                q_refs[slot][...] = query_part

    inner = project(wi).astype(jnp.bfloat16).astype(jnp.float32)
    signal = project(ws).astype(jnp.bfloat16).astype(jnp.float32)
    cin_ref[...] = (inner * signal).astype(jnp.bfloat16)
    gate_ref[...] = project(wo).astype(jnp.bfloat16)


def project_all(sources, member, tokens, gain, cosine, sine, weights, head_dim, heads):
    pieces = len(tokens)
    rows, part_width = tokens[0].shape
    width, columns = weights[0].shape
    lanes = 2 * head_dim
    tile = math.gcd(rows, 256)
    row_block = lambda n: pl.BlockSpec((tile, n), lambda i: (i, 0))
    whole = pl.BlockSpec((width, columns), lambda i: (0, 0))
    shape = lambda n: jax.ShapeDtypeStruct((rows, n), jnp.bfloat16)
    smem = pl.BlockSpec(memory_space=pltpu.SMEM)
    widths = [lanes] * heads + [2 * lanes] * heads + [columns, columns]
    return pl.pallas_call(
        functools.partial(project_kernel, head_dim=head_dim, pieces=pieces, heads=heads),
        grid=(rows // tile,),
        in_specs=[smem, smem] + [row_block(part_width)] * pieces
        + [pl.BlockSpec((pieces, 1, part_width), lambda i: (0, 0, 0)),
           row_block(lanes), row_block(lanes)] + [whole] * 6,
        out_specs=[row_block(n) for n in widths],
        out_shape=[shape(n) for n in widths],
        compiler_params=pltpu.CompilerParams(
            dimension_semantics=("arbitrary",), vmem_limit_bytes=VMEM_BYTES),
        cost_estimate=pl.CostEstimate(
            flops=12 * rows * width * columns, transcendentals=rows,
            bytes_accessed=2 * (rows * width + 6 * width * columns + 5 * rows * columns)),
        name="project",
    )(sources, member, *tokens, gain.reshape(pieces, 1, part_width), cosine, sine, *weights)


def flash_kernel(*refs, members, first, last, head_dim):
    scalar_ref, lambda_ref, q_ref = refs[:3]
    kv_refs = refs[3 : 3 + members]
    rest = refs[3 + members :]
    if not first:
        acc_in, max_in, sum_in = rest[:3]
        rest = rest[3:]
    if last:
        gain_ref, out_ref, totals_ref, acc_ref, max_ref, sum_ref = rest
    else:
        acc_ref, max_ref, sum_ref = rest
    tile = q_ref.shape[0]
    value_dim = 2 * head_dim
    block = kv_refs[0].shape[0]
    step = pl.program_id(0)

    def update():
        queries = q_ref[...] * jnp.asarray(head_dim ** (-0.5), jnp.bfloat16)
        low = lax.broadcasted_iota(jnp.int32, queries.shape, 1) < head_dim
        zero = jnp.zeros_like(queries)
        stacked = jnp.concatenate(
            [jnp.where(low, queries, zero), jnp.where(low, zero, queries)], axis=0
        )
        all_scores = []
        lane_max = None
        for index in range(members):
            scores = lax.dot_general(
                stacked, kv_refs[index][:, :value_dim], (((1,), (1,)), ((), ())),
                preferred_element_type=jnp.float32,
            )
            if first:
                slot = step * tile // block
                row_start = scalar_ref[1 + slot] + step * tile % block
                row_ids = lax.broadcasted_iota(jnp.int32, scores.shape, 0) % tile + row_start
                col_ids = lax.broadcasted_iota(jnp.int32, scores.shape, 1) + scalar_ref[1 + index]
                scores = jnp.where(row_ids >= col_ids, scores, MASKED)
            all_scores.append(scores)
            for g in range(0, block, 128):
                part = scores[:, g : g + 128]
                lane_max = part if lane_max is None else jnp.maximum(lane_max, part)
        row_max = jnp.max(lane_max, axis=1, keepdims=True)
        if not first:
            before = max_in[0][:, :1]
            row_max = jnp.maximum(row_max, before)
            decay = jnp.exp(before - row_max)
        acc = None
        sums = None
        for index in range(members):
            exponent = jnp.exp(all_scores[index] - row_max)
            for g in range(0, block, 128):
                part = exponent[:, g : g + 128]
                sums = part if sums is None else sums + part
            product = jnp.dot(
                exponent.astype(jnp.bfloat16), kv_refs[index][:, value_dim:],
                preferred_element_type=jnp.float32,
            )
            acc = product if acc is None else acc + product
        if not first:
            acc = acc + acc_in[0] * decay
            sums = sums + sum_in[0] * decay
        acc_ref[0] = acc
        sum_ref[0] = sums
        max_ref[0] = jnp.broadcast_to(row_max, sums.shape)

    if first:
        update()
    else:
        pl.when(scalar_ref[0] > 0)(update)

        @pl.when(scalar_ref[0] == 0)
        def _():
            acc_ref[0] = acc_in[0]
            sum_ref[0] = sum_in[0]
            max_ref[0] = max_in[0]

    if last:
        row_max = max_ref[0][:, :1]
        row_sum = jnp.sum(sum_ref[0], axis=1, keepdims=True)
        totals_ref[0] = row_max + jnp.log(row_sum)
        mixed = acc_ref[0] / row_sum
        head_mix = mixed[:tile] - lambda_ref[0] * mixed[tile:]
        mean_square = jnp.mean(head_mix * head_mix, axis=1, keepdims=True)
        normed = head_mix * lax.rsqrt(mean_square + HEAD_EPS) * gain_ref[...] * HEAD_SCALE
        out_ref[...] = normed.astype(jnp.bfloat16)


def flash(scalars, head_lambda, queries, blocks, state, head_gain, last, head_dim):
    rows_all, value_dim = queries.shape
    members = len(blocks)
    block = blocks[0].shape[0]
    tile = math.gcd(block, 256)
    tiles = rows_all // tile
    first = state is None
    smem = pl.BlockSpec(memory_space=pltpu.SMEM)
    state_spec = pl.BlockSpec((1, 2 * tile, value_dim), lambda i: (i, 0, 0))
    state_shape = jax.ShapeDtypeStruct((tiles, 2 * tile, value_dim), jnp.float32)
    q_spec = pl.BlockSpec((tile, value_dim), lambda i: (i, 0))
    in_specs = [smem, smem, q_spec]
    in_specs += [pl.BlockSpec((block, 2 * value_dim), lambda i: (0, 0))] * members
    args = [scalars, head_lambda, queries, *blocks]
    if not first:
        in_specs += [state_spec] * 3
        args += list(state)
    if last:
        in_specs.append(pl.BlockSpec((1, value_dim), lambda i: (0, 0)))
        args.append(head_gain)
        out_specs = [q_spec, pl.BlockSpec((1, 2 * tile, 1), lambda i: (i, 0, 0))]
        out_shape = [
            jax.ShapeDtypeStruct((rows_all, value_dim), jnp.bfloat16),
            jax.ShapeDtypeStruct((tiles, 2 * tile, 1), jnp.float32),
        ]
        scratch = [pltpu.VMEM((1, 2 * tile, value_dim), jnp.float32)] * 3
    else:
        out_specs = [state_spec] * 3
        out_shape = [state_shape] * 3
        scratch = []
    pairs = rows_all * block * members
    return pl.pallas_call(
        functools.partial(
            flash_kernel, members=members, first=first, last=last, head_dim=head_dim
        ),
        grid=(tiles,),
        in_specs=in_specs,
        out_specs=out_specs,
        out_shape=out_shape,
        scratch_shapes=scratch,
        compiler_params=pltpu.CompilerParams(
            dimension_semantics=("arbitrary",), vmem_limit_bytes=VMEM_BYTES),
        cost_estimate=pl.CostEstimate(
            flops=32 * pairs * value_dim, transcendentals=2 * pairs,
            bytes_accessed=24 * rows_all * value_dim),
        name="flash",
    )(*args)


def merge_kernel(*refs, pieces, with_base):
    source_ref = refs[0]
    parts = refs[1 : 1 + pieces]
    weight_ref = refs[1 + pieces]
    out_ref = refs[-1]
    depth = parts[0].shape[1]
    total = refs[2 + pieces][...] if with_base else None
    for index in range(pieces):
        start = pl.multiple_of(source_ref[index] * depth, depth)
        product = jnp.dot(
            parts[index][...], weight_ref[pl.ds(start, depth), :],
            preferred_element_type=jnp.float32,
        )
        total = product if total is None else total + product
    out_ref[...] = total.astype(out_ref.dtype)


def merge(sources, parts, weight, base):
    rows, depth = parts[0].shape
    columns = weight.shape[1]
    tile = math.gcd(rows, 256)
    row_block = lambda n: pl.BlockSpec((tile, n), lambda i: (i, 0))
    with_base = base is not None
    return pl.pallas_call(
        functools.partial(merge_kernel, pieces=len(parts), with_base=with_base),
        grid=(rows // tile,),
        in_specs=[pl.BlockSpec(memory_space=pltpu.SMEM)] + [row_block(depth)] * len(parts)
        + [pl.BlockSpec(weight.shape, lambda i: (0, 0))] + [row_block(columns)] * with_base,
        out_specs=row_block(columns),
        out_shape=jax.ShapeDtypeStruct((rows, columns), jnp.bfloat16 if with_base else jnp.float32),
        compiler_params=pltpu.CompilerParams(
            dimension_semantics=("arbitrary",), vmem_limit_bytes=VMEM_BYTES),
        cost_estimate=pl.CostEstimate(
            flops=2 * rows * weight.shape[0] * columns, transcendentals=0,
            bytes_accessed=2 * weight.shape[0] * (rows + columns) + 4 * rows * columns),
        name="merge",
    )(sources, *parts, weight, *([base] if with_base else []))


def per_device(
    tokens,
    norm_gain,
    query_weight,
    key_weight,
    value_weight,
    outer_gate_weight,
    inner_gate_weight,
    conv_input_weight,
    conv_taps,
    lambdas,
    head_gain,
    attn_out_weight,
    conv_out_weight,
):
    local_rows = tokens.shape[0]
    heads = lambdas.shape[0]
    head_dim = query_weight.shape[1] // (2 * heads)
    taps_count = conv_taps.shape[0]
    columns_dev = query_weight.shape[1]
    sp_size = lax.axis_size("sp")
    groups = sp_size // heads
    place = lax.axis_index("sp").astype(jnp.int32)
    group, member = place // heads, place % heads
    positions = (
        place * local_rows + jnp.arange(local_rows, dtype=jnp.int32)
    ).astype(jnp.float32)
    cosine, sine = turn_tables(positions, head_dim, 2 * head_dim)
    token_parts, sources = tp_pieces(tokens)
    sources = jnp.stack(sources)
    projected = project_all(
        sources, member[None], token_parts, norm_gain, cosine, sine,
        (query_weight, key_weight, value_weight, outer_gate_weight,
         inner_gate_weight, conv_input_weight),
        head_dim, heads,
    )
    query_slots, block_slots = projected[:heads], projected[heads : 2 * heads]
    conv_in, outer_gate = projected[2 * heads :]

    def to_member(block, distance):
        route = [
            (g * heads + m, g * heads + (m + distance) % heads)
            for g in range(groups) for m in range(heads)
        ]
        return lax.ppermute(block, "sp", route)

    def up(block):
        route = [(i, i + heads) for i in range(sp_size - heads)]
        return lax.ppermute(block, "sp", route)

    blocks = [block_slots[0]] + [to_member(block_slots[k], k) for k in range(1, heads)]
    queries = [query_slots[0]] + [to_member(query_slots[k], k) for k in range(1, heads)]
    queries = jnp.concatenate(queries, axis=0) if heads > 1 else queries[0]
    offsets = [((member - k) % heads) * local_rows for k in range(heads)]
    head_lambda = lax.dynamic_slice_in_dim(lambdas, member, 1, 0)

    rim_rows = shifted(conv_in[local_rows - (taps_count - 1) :], "sp", 1)
    padded = jnp.concatenate([rim_rows, conv_in], axis=0)
    summed = jnp.zeros((local_rows, columns_dev), jnp.float32)
    for tap_index in range(taps_count):
        summed = summed + conv_taps[tap_index][None, :] * padded[
            tap_index : tap_index + local_rows
        ].astype(jnp.float32)
    conv_out = (outer_gate.astype(jnp.float32) * summed).astype(jnp.bfloat16)
    conv_parts, unused = tp_pieces(conv_out)
    conv_part = merge(sources, conv_parts, conv_out_weight, None)

    state = None
    for step in range(groups):
        scalars = jnp.stack([(group >= step).astype(jnp.int32)] + offsets)
        arriving = [up(block) for block in blocks] if step + 1 < groups else None
        state = flash(
            scalars, head_lambda, queries, blocks, state, head_gain[None, :],
            step + 1 == groups, head_dim,
        )
        blocks = arriving
        if step == min(1, groups - 2):
            state, conv_part = lax.optimization_barrier((state, conv_part))
    mixes, totals = state
    tile = mixes.shape[0] // totals.shape[0]
    totals = totals.reshape(heads, local_rows // tile, 2, tile).transpose(0, 2, 1, 3)
    totals = totals.reshape(heads, 2, local_rows)
    mixes = mixes.reshape(heads, local_rows, 2 * head_dim)
    home_mix = [mixes[0]] + [to_member(mixes[k], heads - k) for k in range(1, heads)]
    home_totals = [totals[0]] + [to_member(totals[k], heads - k) for k in range(1, heads)]

    def in_order(slots, axis, join):
        result = join([slots[h] for h in range(heads)], axis)
        for m in range(1, heads):
            turned = join([slots[(h - m) % heads] for h in range(heads)], axis)
            result = jnp.where(member == m, turned, result)
        return result

    attn_out = in_order(home_mix, 1, jnp.concatenate)
    log_totals = in_order(home_totals, 0, jnp.stack)
    attn_parts, unused = tp_pieces(attn_out)
    mixed_out = merge(sources, attn_parts, attn_out_weight, conv_part)
    return (mixed_out, log_totals)


def solution(mesh):
    in_specs = (
        P("sp", "tp"),
        P(),
        P(None, "tp"),
        P(None, "tp"),
        P(None, "tp"),
        P(None, "tp"),
        P(None, "tp"),
        P(None, "tp"),
        P(None, "tp"),
        P("tp"),
        P(),
        P(None, "tp"),
        P(None, "tp"),
    )
    out_specs = (P("sp", "tp"), P("tp", None, "sp"))
    return jax.shard_map(
        per_device, mesh=mesh, in_specs=in_specs, out_specs=out_specs, check_vma=False
    )
```

```python
import functools
import math

import jax
import jax.numpy as jnp
from jax import lax
from jax.experimental import pallas as pl
from jax.experimental.pallas import tpu as pltpu
from jax.sharding import PartitionSpec as P

NORM_EPS = 1e-06
HEAD_EPS = 1e-05
ROPE_BASE = 500000.0
MASKED = -1e30
HEAD_SCALE = 0.8
MIB = 1024 * 1024


FLASH_TILE = 256
FLASH_ROWS = 256


def shifted(block, axis, distance):
    devices = range(lax.axis_size(axis))
    route = [(i - distance, i) for i in devices if i - distance in devices]
    return lax.ppermute(block, axis, route)


def turn_tables(positions, head_dim, columns):
    half_dim = head_dim // 2
    frequency = ROPE_BASE ** (-jnp.arange(half_dim, dtype=jnp.float32) * 2.0 / head_dim)
    angles = positions[:, None] * jnp.tile(frequency, columns // half_dim)[None, :]
    sign = jnp.where((jnp.arange(columns) % head_dim) < half_dim, -1.0, 1.0)
    return jnp.cos(angles), jnp.sin(angles) * sign[None, :]


def tp_pieces(block):
    size = lax.axis_size("tp")
    here = lax.axis_index("tp").astype(jnp.int32)
    if size == 4:
        far = lax.ppermute(block, "tp", [(i, i ^ 2) for i in range(4)])
        near = lax.ppermute(block, "tp", [(i, i ^ 1) for i in range(4)])
        both = lax.ppermute(far, "tp", [(i, i ^ 1) for i in range(4)])
        return [block, near, far, both], [here, here ^ 1, here ^ 2, here ^ 3]
    gathered = lax.all_gather(block, "tp", axis=0, tiled=False)
    return [gathered[i] for i in range(size)], [jnp.int32(i) for i in range(size)]


def project_kernel(*refs, head_dim, pieces, heads):
    source_ref, member_ref = refs[:2]
    tokens = refs[2 : 2 + pieces]
    gain_ref, cos_ref, sin_ref, wq, wk, wv, wo, wi, ws = refs[2 + pieces : 11 + pieces]
    outs = refs[11 + pieces :]
    q_refs, kv_refs = outs[:heads], outs[heads : 2 * heads]
    cin_ref, gate_ref = outs[2 * heads :]
    part_width = tokens[0].shape[1]
    width = part_width * pieces
    rows = tokens[0].shape[0]
    squares = jnp.zeros((rows, 1), jnp.float32)
    scaled = []
    windows = []
    for index in range(pieces):
        start = pl.multiple_of(source_ref[index] * part_width, part_width)
        floats = tokens[index][...].astype(jnp.float32)
        squares = squares + jnp.sum(floats * floats, axis=1, keepdims=True)
        gain = gain_ref[source_ref[index]]
        scaled.append((floats * gain).astype(jnp.bfloat16))
        windows.append(pl.ds(start, part_width))
    inverse_rms = lax.rsqrt(squares / width + NORM_EPS)
    lanes = 2 * head_dim
    half = head_dim // 2

    def project(w):
        total = jnp.dot(scaled[0], w[windows[0], :], preferred_element_type=jnp.float32)
        for index in range(1, pieces):
            total = total + jnp.dot(
                scaled[index], w[windows[index], :], preferred_element_type=jnp.float32
            )
        return total * inverse_rms

    low = lax.broadcasted_iota(jnp.int32, (rows, lanes), 1) % head_dim < half
    cosine = cos_ref[...]
    sine = sin_ref[...]

    def turned(part):
        other = jnp.where(low, pltpu.roll(part, lanes - half, 1), pltpu.roll(part, half, 1))
        return (part * cosine + other * sine).astype(jnp.bfloat16)

    keys = project(wk)
    values = project(wv).astype(jnp.bfloat16)
    queries = project(wq)
    for head in range(heads):
        columns = slice(head * lanes, (head + 1) * lanes)
        key_part = turned(keys[:, columns])
        query_part = turned(queries[:, columns])
        value_part = values[:, columns]
        for slot in range(heads):

            @pl.when((member_ref[0] + slot) % heads == head)
            def _():
                kv_refs[slot][:, :lanes] = key_part
                kv_refs[slot][:, lanes:] = value_part
                q_refs[slot][...] = query_part

    inner = project(wi).astype(jnp.bfloat16).astype(jnp.float32)
    signal = project(ws).astype(jnp.bfloat16).astype(jnp.float32)
    cin_ref[...] = (inner * signal).astype(jnp.bfloat16)
    gate_ref[...] = project(wo).astype(jnp.bfloat16)


def project_all(sources, member, tokens, gain, cosine, sine, weights, head_dim, heads):
    pieces = len(tokens)
    rows, part_width = tokens[0].shape
    width, columns = weights[0].shape
    lanes = 2 * head_dim
    tile = math.gcd(rows, 256)
    row_block = lambda n: pl.BlockSpec((tile, n), lambda i: (i, 0))
    whole = pl.BlockSpec((width, columns), lambda i: (0, 0))
    shape = lambda n: jax.ShapeDtypeStruct((rows, n), jnp.bfloat16)
    smem = pl.BlockSpec(memory_space=pltpu.SMEM)
    widths = [lanes] * heads + [2 * lanes] * heads + [columns, columns]
    return pl.pallas_call(
        functools.partial(project_kernel, head_dim=head_dim, pieces=pieces, heads=heads),
        grid=(rows // tile,),
        in_specs=[smem, smem] + [row_block(part_width)] * pieces
        + [pl.BlockSpec((pieces, 1, part_width), lambda i: (0, 0, 0)),
           row_block(lanes), row_block(lanes)] + [whole] * 6,
        out_specs=[row_block(n) for n in widths],
        out_shape=[shape(n) for n in widths],
        compiler_params=pltpu.CompilerParams(
            dimension_semantics=("arbitrary",), vmem_limit_bytes=28 * MIB),
        cost_estimate=pl.CostEstimate(
            flops=12 * rows * width * columns, transcendentals=rows,
            bytes_accessed=2 * (rows * width + 6 * width * columns + 5 * rows * columns)),
        name="project",
    )(sources, member, *tokens, gain.reshape(pieces, 1, part_width), cosine, sine, *weights)


def flash_kernel(*refs, members, first, last, head_dim, chunk):
    scalar_ref, lambda_ref, q_ref = refs[:3]
    kv_refs = refs[3 : 3 + members]
    rest = refs[3 + members :]
    if not first:
        acc_in, stat_in = rest[:2]
        rest = rest[2:]
    if last:
        gain_ref, out_ref, totals_ref, acc_ref, stat_ref = rest
    else:
        acc_ref, stat_ref = rest
    tile = q_ref.shape[0]
    value_dim = 2 * head_dim
    block = kv_refs[0].shape[0]
    step = pl.program_id(0)

    def update():
        queries = q_ref[...] * jnp.asarray(head_dim ** (-0.5), jnp.bfloat16)
        low = lax.broadcasted_iota(jnp.int32, queries.shape, 1) < head_dim
        zero = jnp.zeros_like(queries)
        stacked = jnp.concatenate(
            [jnp.where(low, queries, zero), jnp.where(low, zero, queries)], axis=0
        )
        waiting = scores_of(stacked[:chunk], 0)
        for r in range(chunk, 2 * tile, chunk):
            following = scores_of(stacked[r : r + chunk], r)
            finish(waiting, r - chunk)
            waiting = following
        finish(waiting, 2 * tile - chunk)

    def scores_of(part_rows, r):
        all_scores = []
        lane_max = None
        for index in range(members):
            scores = lax.dot_general(
                part_rows, kv_refs[index][:, :value_dim], (((1,), (1,)), ((), ())),
                preferred_element_type=jnp.float32,
            )
            if first:
                slot = step * tile // block
                row_start = scalar_ref[1 + slot] + step * tile % block + r % tile
                row_ids = lax.broadcasted_iota(jnp.int32, scores.shape, 0) + row_start
                col_ids = lax.broadcasted_iota(jnp.int32, scores.shape, 1) + scalar_ref[1 + index]
                scores = jnp.where(row_ids >= col_ids, scores, MASKED)
            all_scores.append(scores)
            for g in range(0, block, 128):
                part = scores[:, g : g + 128]
                lane_max = part if lane_max is None else jnp.maximum(lane_max, part)
        return all_scores, lane_max

    def finish(scored, r):
        all_scores, lane_max = scored
        rows = slice(r, r + chunk)
        row_max = jnp.max(lane_max, axis=1, keepdims=True)
        if not first:
            before = stat_in[0, rows, :1]
            row_max = jnp.maximum(row_max, before)
            decay = jnp.exp(before - row_max)
        acc = None
        sums = None
        for index in range(members):
            exponent = jnp.exp(all_scores[index] - row_max)
            for g in range(0, block, 128):
                part = exponent[:, g : g + 128]
                sums = part if sums is None else sums + part
            product = jnp.dot(
                exponent.astype(jnp.bfloat16), kv_refs[index][:, value_dim:],
                preferred_element_type=jnp.float32,
            )
            acc = product if acc is None else acc + product
        if not first:
            acc = acc + acc_in[0, rows] * decay
        row_sum = jnp.sum(sums, axis=1, keepdims=True)
        if not first:
            row_sum = row_sum + stat_in[0, rows, head_dim : head_dim + 1] * decay
        acc_ref[0, rows] = acc
        low = lax.broadcasted_iota(jnp.int32, acc.shape, 1) < head_dim
        stat_ref[0, rows] = jnp.where(low, row_max, row_sum)

    if first:
        update()
    else:
        pl.when(scalar_ref[0] > 0)(update)

        @pl.when(scalar_ref[0] == 0)
        def _():
            acc_ref[0] = acc_in[0]
            stat_ref[0] = stat_in[0]

    if last:
        row_max = stat_ref[0, :, :1]
        row_sum = stat_ref[0, :, head_dim : head_dim + 1]
        totals_ref[0] = row_max + jnp.log(row_sum)
        mixed = acc_ref[0] / row_sum
        head_mix = mixed[:tile] - lambda_ref[0] * mixed[tile:]
        mean_square = jnp.mean(head_mix * head_mix, axis=1, keepdims=True)
        normed = head_mix * lax.rsqrt(mean_square + HEAD_EPS) * gain_ref[...] * HEAD_SCALE
        out_ref[...] = normed.astype(jnp.bfloat16)


def flash(scalars, head_lambda, queries, blocks, state, head_gain, last, head_dim):
    rows_all, value_dim = queries.shape
    members = len(blocks)
    block = blocks[0].shape[0]
    tile = math.gcd(block, FLASH_TILE)
    tiles = rows_all // tile
    first = state is None
    smem = pl.BlockSpec(memory_space=pltpu.SMEM)
    state_spec = pl.BlockSpec((1, 2 * tile, value_dim), lambda i: (i, 0, 0))
    state_shape = jax.ShapeDtypeStruct((tiles, 2 * tile, value_dim), jnp.float32)
    q_spec = pl.BlockSpec((tile, value_dim), lambda i: (i, 0))
    in_specs = [smem, smem, q_spec]
    in_specs += [pl.BlockSpec((block, 2 * value_dim), lambda i: (0, 0))] * members
    args = [scalars, head_lambda, queries, *blocks]
    if not first:
        in_specs += [state_spec] * 2
        args += list(state)
    if last:
        in_specs.append(pl.BlockSpec((1, value_dim), lambda i: (0, 0)))
        args.append(head_gain)
        out_specs = [q_spec, pl.BlockSpec((1, 2 * tile, 1), lambda i: (i, 0, 0))]
        out_shape = [
            jax.ShapeDtypeStruct((rows_all, value_dim), jnp.bfloat16),
            jax.ShapeDtypeStruct((tiles, 2 * tile, 1), jnp.float32),
        ]
        scratch = [pltpu.VMEM((1, 2 * tile, value_dim), jnp.float32)] * 2
    else:
        out_specs = [state_spec] * 2
        out_shape = [state_shape] * 2
        scratch = []
    pairs = rows_all * block * members
    return pl.pallas_call(
        functools.partial(
            flash_kernel, members=members, first=first, last=last, head_dim=head_dim,
            chunk=math.gcd(tile, FLASH_ROWS),
        ),
        grid=(tiles,),
        in_specs=in_specs,
        out_specs=out_specs,
        out_shape=out_shape,
        scratch_shapes=scratch,
        compiler_params=pltpu.CompilerParams(
            dimension_semantics=("arbitrary",), vmem_limit_bytes=20 * MIB),
        cost_estimate=pl.CostEstimate(
            flops=32 * pairs * value_dim, transcendentals=2 * pairs,
            bytes_accessed=24 * rows_all * value_dim),
        name="flash",
    )(*args)


def merge_kernel(*refs, pieces, with_base):
    source_ref = refs[0]
    parts = refs[1 : 1 + pieces]
    weight_ref = refs[1 + pieces]
    out_ref = refs[-1]
    depth = parts[0].shape[1]
    total = refs[2 + pieces][...] if with_base else None
    for index in range(pieces):
        start = pl.multiple_of(source_ref[index] * depth, depth)
        product = jnp.dot(
            parts[index][...], weight_ref[pl.ds(start, depth), :],
            preferred_element_type=jnp.float32,
        )
        total = product if total is None else total + product
    out_ref[...] = total.astype(out_ref.dtype)


def merge(sources, parts, weight, base):
    rows, depth = parts[0].shape
    columns = weight.shape[1]
    tile = math.gcd(rows, 256)
    row_block = lambda n: pl.BlockSpec((tile, n), lambda i: (i, 0))
    with_base = base is not None
    return pl.pallas_call(
        functools.partial(merge_kernel, pieces=len(parts), with_base=with_base),
        grid=(rows // tile,),
        in_specs=[pl.BlockSpec(memory_space=pltpu.SMEM)] + [row_block(depth)] * len(parts)
        + [pl.BlockSpec(weight.shape, lambda i: (0, 0))] + [row_block(columns)] * with_base,
        out_specs=row_block(columns),
        out_shape=jax.ShapeDtypeStruct((rows, columns), jnp.bfloat16 if with_base else jnp.float32),
        compiler_params=pltpu.CompilerParams(
            dimension_semantics=("arbitrary",), vmem_limit_bytes=12 * MIB),
        cost_estimate=pl.CostEstimate(
            flops=2 * rows * weight.shape[0] * columns, transcendentals=0,
            bytes_accessed=2 * weight.shape[0] * (rows + columns) + 4 * rows * columns),
        name="merge",
    )(sources, *parts, weight, *([base] if with_base else []))


def per_device(
    tokens,
    norm_gain,
    query_weight,
    key_weight,
    value_weight,
    outer_gate_weight,
    inner_gate_weight,
    conv_input_weight,
    conv_taps,
    lambdas,
    head_gain,
    attn_out_weight,
    conv_out_weight,
):
    local_rows = tokens.shape[0]
    heads = lambdas.shape[0]
    head_dim = query_weight.shape[1] // (2 * heads)
    taps_count = conv_taps.shape[0]
    columns_dev = query_weight.shape[1]
    sp_size = lax.axis_size("sp")
    groups = sp_size // heads
    place = lax.axis_index("sp").astype(jnp.int32)
    group, member = place // heads, place % heads
    positions = (
        place * local_rows + jnp.arange(local_rows, dtype=jnp.int32)
    ).astype(jnp.float32)
    cosine, sine = turn_tables(positions, head_dim, 2 * head_dim)
    token_parts, sources = tp_pieces(tokens)
    sources = jnp.stack(sources)
    projected = project_all(
        sources, member[None], token_parts, norm_gain, cosine, sine,
        (query_weight, key_weight, value_weight, outer_gate_weight,
         inner_gate_weight, conv_input_weight),
        head_dim, heads,
    )
    query_slots, block_slots = projected[:heads], projected[heads : 2 * heads]
    conv_in, outer_gate = projected[2 * heads :]

    def to_member(block, distance):
        route = [
            (g * heads + m, g * heads + (m + distance) % heads)
            for g in range(groups) for m in range(heads)
        ]
        return lax.ppermute(block, "sp", route)

    def up(block):
        route = [(i, i + heads) for i in range(sp_size - heads)]
        return lax.ppermute(block, "sp", route)

    blocks = [block_slots[0]] + [to_member(block_slots[k], k) for k in range(1, heads)]
    queries = [query_slots[0]] + [to_member(query_slots[k], k) for k in range(1, heads)]
    queries = jnp.concatenate(queries, axis=0) if heads > 1 else queries[0]
    offsets = [((member - k) % heads) * local_rows for k in range(heads)]
    head_lambda = lax.dynamic_slice_in_dim(lambdas, member, 1, 0)

    rim_rows = shifted(conv_in[local_rows - (taps_count - 1) :], "sp", 1)
    padded = jnp.concatenate([rim_rows, conv_in], axis=0)
    summed = jnp.zeros((local_rows, columns_dev), jnp.float32)
    for tap_index in range(taps_count):
        summed = summed + conv_taps[tap_index][None, :] * padded[
            tap_index : tap_index + local_rows
        ].astype(jnp.float32)
    conv_out = (outer_gate.astype(jnp.float32) * summed).astype(jnp.bfloat16)
    conv_parts, unused = tp_pieces(conv_out)
    conv_part = merge(sources, conv_parts, conv_out_weight, None)

    state = None
    for step in range(groups):
        scalars = jnp.stack([(group >= step).astype(jnp.int32)] + offsets)
        arriving = [up(block) for block in blocks] if step + 1 < groups else None
        state = flash(
            scalars, head_lambda, queries, blocks, state, head_gain[None, :],
            step + 1 == groups, head_dim,
        )
        blocks = arriving
        if step == min(1, groups - 2):
            state, conv_part = lax.optimization_barrier((state, conv_part))
    mixes, totals = state
    tile = mixes.shape[0] // totals.shape[0]
    totals = totals.reshape(heads, local_rows // tile, 2, tile).transpose(0, 2, 1, 3)
    totals = totals.reshape(heads, 2, local_rows)
    mixes = mixes.reshape(heads, local_rows, 2 * head_dim)
    home_mix = [mixes[0]] + [to_member(mixes[k], heads - k) for k in range(1, heads)]
    home_totals = [totals[0]] + [to_member(totals[k], heads - k) for k in range(1, heads)]

    def in_order(slots, axis, join):
        result = join([slots[h] for h in range(heads)], axis)
        for m in range(1, heads):
            turned = join([slots[(h - m) % heads] for h in range(heads)], axis)
            result = jnp.where(member == m, turned, result)
        return result

    attn_out = in_order(home_mix, 1, jnp.concatenate)
    log_totals = in_order(home_totals, 0, jnp.stack)
    attn_parts, unused = tp_pieces(attn_out)
    mixed_out = merge(sources, attn_parts, attn_out_weight, conv_part)
    return (mixed_out, log_totals)


def solution(mesh):
    in_specs = (
        P("sp", "tp"),
        P(),
        P(None, "tp"),
        P(None, "tp"),
        P(None, "tp"),
        P(None, "tp"),
        P(None, "tp"),
        P(None, "tp"),
        P(None, "tp"),
        P("tp"),
        P(),
        P(None, "tp"),
        P(None, "tp"),
    )
    out_specs = (P("sp", "tp"), P("tp", None, "sp"))
    return jax.shard_map(
        per_device, mesh=mesh, in_specs=in_specs, out_specs=out_specs, check_vma=False
    )
```
